32 devices in a mesh: ep: 8 (over z, core), tp: 4 (over y, x).
Axes of the slice: x: 2, y: 2, z: 4, core: 2. Of those that a mesh axis runs over, the one named last changes fastest.
Arguments:
- tokens: bfloat16 [2048, 4096], P('ep', 'tp'), may hold values from -2000 to 2000, as said below
- norm_gain: float32 [4096], P('tp'), may hold values from 0.1 to 1.9
- route_ids: int32 [2048, 2], P('ep'), may hold values from 0 to 15, all different within a row; in each aligned block of 256 rows (0 to 255, 256 to 511, ...) at most 40 rows name the same one
- route_gates: float32 [2048, 2], P('ep'), may hold values from 0.1 to 1
- w_gate: bfloat16 [16, 768, 4096], P('ep', None, 'tp'), may hold values from -0.09375 to 0.09375
- w_up: bfloat16 [16, 768, 4096], P('ep', None, 'tp'), may hold values from -0.09375 to 0.09375
- w_down: bfloat16 [16, 768, 4096], P('ep', None, 'tp'), may hold values from -0.21875 to 0.21875
Outputs:
- mixed: bfloat16 [2048, 4096], P('ep', 'tp')
The draws below stay inside these ranges and needn't reach their ends.
Inputs may be any that keep to these rules, and one draw needn't show every extreme that they name: `route_ids`: each row names 2 different experts; among the 256 rows of one index of ep no expert is named by more than 40 rows, a bound that some block reaches. `tokens`: finite values.
All inputs are finite; a program needn't handle non-finite values.
Results may differ from the reference program's by a relative error of at most 0.025.
Values may be sent and summed in bfloat16 or wider, within the bound.
A program may use at most 64 MiB of HBM per device.

```python
import math
import jax
import jax.numpy as jnp
import numpy as np
from jax import lax

D = 4096
FF = 768
TOK_EP = 256
TOP_K = 2
EXPERTS = 16
TOKENS = 2048
CAP = 40
N_EP = 8
N_TP = 4


def draw_tokens(key, part):
    first, second, third = jax.random.split(jax.random.fold_in(key, 11), 3)
    columns = jnp.arange(D, dtype=jnp.float32)
    col_scale = 3.0 ** (columns / D) * jnp.exp(jax.random.uniform(second, (D,), jnp.float32) * math.log(4.0))
    row_scale = jnp.exp(jax.random.uniform(third, (TOKENS, 1), jnp.float32) * math.log(10.0))
    base = jax.random.normal(first, (TOKENS, D), jnp.float32)
    return (base * row_scale * col_scale[None, :]).astype(jnp.bfloat16)


def levels(rng, shape, cuts, low, largest):
    level, own = 1.0, jax.random.fold_in(rng, 6)
    for position, shards_of in cuts:
        steps = jnp.exp(jax.random.uniform(jax.random.fold_in(own, position), (shards_of,), jnp.float32, low / len(cuts), largest / len(cuts)))
        level = level * jnp.repeat(steps, shape[position] // shards_of).reshape([-1 if axis == position else 1 for axis in range(len(shape))])
    return level


def shared_out(key, own, number, rows, count, top, most, lean):
    ranking = jax.random.permutation(key, count)
    heavy_load, common = portions_of(count, rows * top, most, lean, True), portions_of(count, rows * top, most, lean, False)
    places = jnp.arange(count)

    def named(tallies, turn):
        used = int((tallies > 0).sum())
        fixed = max(1, used // 4)
        moved = fixed + (places - fixed + turn * (used - fixed)) % max(1, count - fixed)
        return jnp.zeros((count,), jnp.int32).at[ranking[jnp.where(places < fixed, places, moved)]].set(jnp.asarray(tallies, jnp.int32))

    tallies = jnp.where(number % 4 == 0, named(heavy_load, number // 4), named(common, number - number // 4 - 1))
    mixed = jax.random.permutation(jax.random.fold_in(own, 3), count)
    donor, receiver = mixed[0:count // 2 * 2:2], mixed[1:count // 2 * 2:2]
    margin = jnp.minimum(tallies[donor] - 1, most - tallies[receiver]) // 2
    margin = jnp.where((donor == ranking[0]) | (receiver == ranking[0]) | (tallies[receiver] == 0), 0, jnp.maximum(margin, 0))
    moved = jax.random.randint(jax.random.fold_in(own, 4), (count // 2,), 0, 1 << 20) % (margin + 1)
    tallies = tallies.at[donor].add(-moved).at[receiver].add(moved)
    items = jnp.searchsorted(jnp.cumsum(tallies), jnp.arange(rows * top), side="right").astype(jnp.int32)
    grid = items.reshape(top, rows).T
    grid = grid[jax.random.permutation(jax.random.fold_in(own, 1), rows)]
    turn = jax.random.randint(jax.random.fold_in(own, 2), (rows, 1), 0, top)
    return jnp.take_along_axis(grid, (jnp.arange(top)[None, :] + turn) % top, axis=1)


def portions_of(amount, total, reach, skew, full):
    portions = [(1 << 20) // math.isqrt(standing ** skew) + 1 for standing in range(1, amount + 1)]
    largest = reach if full else min(reach, max(-(-total // amount), total * portions[0] // sum(portions)))
    least = 1 if total - largest >= amount - 1 else 0
    holding, surplus = [largest] + [least] * (amount - 1), total - largest - least * (amount - 1)
    while surplus > 0:
        free = [i for i in range(1, amount) if holding[i] < largest] or [i for i in range(1, amount) if holding[i] < reach]
        whole, left = sum([portions[i] for i in free]), surplus
        for i in free:
            addition = min(reach - holding[i], max(1, left * portions[i] // whole), surplus)
            holding[i] = holding[i] + addition
            surplus = surplus - addition
    return np.array(holding)


def normal_values(own_key, extent, spread, reach, cuts=(), held_as=jnp.bfloat16):
    entries = spread * jax.random.normal(own_key, extent, jnp.float32)
    if cuts:
        entries = entries * levels(own_key, extent, cuts, -0.22, 0.18)
    return jnp.clip(entries, -reach, reach).astype(held_as)


def setup_inputs(seed: int = 0) -> dict:
    seeds = jax.random.split(jax.random.key(seed), 8)
    tokens = draw_tokens(jax.random.fold_in(seeds[7], 71), 0)
    norm_gain = jnp.clip(1.0 + 0.18 * jax.random.normal(seeds[1], (D,), jnp.float32), 0.1, 1.9)
    route_ids_keys = jax.random.split(jax.random.fold_in(seeds[2], 1), TOKENS // TOK_EP)
    route_ids_turns = jax.random.permutation(jax.random.fold_in(seeds[2], 3), TOKENS // TOK_EP)
    route_ids = jax.vmap(lambda own, number: shared_out(jax.random.fold_in(seeds[2], 2), own, number, TOK_EP, EXPERTS, TOP_K, CAP, 2))(route_ids_keys, route_ids_turns).reshape((TOKENS, TOP_K))
    route_gates = jnp.clip(0.1 + 0.9 * jax.random.uniform(seeds[3], (TOKENS, TOP_K), jnp.float32) ** levels(seeds[3], (TOKENS, TOP_K), ((0, 8),), -0.2, 0.2), 0.1, 1.0)
    w_gate = normal_values(seeds[4], (EXPERTS, FF, D), D ** -0.5, 0.09375, ((0, 8), (2, 4)))
    w_up = normal_values(seeds[5], (EXPERTS, FF, D), D ** -0.5, 0.09375, ((0, 8), (2, 4)))
    w_down = normal_values(seeds[6], (EXPERTS, FF, D), FF ** -0.5, 0.21875, ((0, 8), (2, 4)))
    return {"tokens": tokens, "norm_gain": norm_gain, "route_ids": route_ids, "route_gates": route_gates, "w_gate": w_gate, "w_up": w_up, "w_down": w_down}


EPSILON = 1e-06

def split_product(rows, weight):
    width = rows.shape[1] // N_TP
    blocks = rows.astype(jnp.float32).reshape(rows.shape[0], N_TP, width)
    wblocks = weight.astype(jnp.float32).reshape(weight.shape[0], N_TP, width)
    partial_value = jnp.einsum('rnc,fnc->nrf', blocks, wblocks)
    return lax.optimization_barrier(jnp.sum(partial_value.astype(jnp.bfloat16).astype(jnp.float32), axis=0))

def reference(tokens, norm_gain, route_ids, route_gates, w_gate, w_up, w_down):
    values = tokens.astype(jnp.float32)
    inverse = lax.rsqrt(lax.optimization_barrier(jnp.mean(values * values, axis=1, keepdims=True)) + EPSILON)
    normed = (values * inverse * norm_gain[None, :]).astype(jnp.bfloat16)
    total_tok = tokens.shape[0]
    flat_ids = route_ids.reshape(N_EP, TOK_EP * TOP_K).astype(jnp.int32)
    onehot = (flat_ids[:, :, None] == jnp.arange(EXPERTS, dtype=jnp.int32)[None, None, :]).astype(jnp.int32)
    before = jnp.cumsum(onehot, axis=1) - onehot
    slot_of = lax.optimization_barrier(jnp.sum(before * onehot, axis=2))
    source = jnp.arange(N_EP, dtype=jnp.int32)[:, None]
    target = ((flat_ids * N_EP + source) * CAP + slot_of).reshape(-1).astype(jnp.int32)
    owners = jnp.repeat(jnp.arange(total_tok, dtype=jnp.int32), TOP_K)
    table = jnp.full((EXPERTS * N_EP * CAP,), total_tok, jnp.int32).at[target].set(owners)
    padded = jnp.concatenate([normed, jnp.zeros((1, D), jnp.bfloat16)], axis=0)

    def run_expert(inputs):
        index_rows, gate_w, up_w, down_w = inputs
        gathered = padded[index_rows]
        gate_act = split_product(gathered, gate_w)
        up_act = split_product(gathered, up_w)
        hidden = (jax.nn.silu(gate_act) * up_act).astype(jnp.bfloat16)
        return jnp.dot(hidden, down_w, preferred_element_type=jnp.float32).astype(jnp.bfloat16)
    outputs = lax.map(run_expert, (table.reshape(EXPERTS, N_EP * CAP), w_gate, w_up, w_down))
    picked = outputs.reshape(EXPERTS * N_EP * CAP, D)[target]
    weighted = picked.astype(jnp.float32).reshape(total_tok, TOP_K, D) * route_gates.astype(jnp.float32)[:, :, None]
    return lax.optimization_barrier(jnp.sum(weighted, axis=1)).astype(jnp.bfloat16)
```

```python
import functools

import jax
import jax.numpy as jnp
from jax import lax
from jax.experimental import pallas as pl
from jax.experimental.pallas import tpu as pltpu
from jax.sharding import PartitionSpec as P

EPSILON = 1e-06
MESH = pl.DeviceIdType.MESH
OWN_CHIP, REMOTE, NEXT_CHIP = range(3)


def gate_up_term(arrived, gate_w, up_w):

    def term(start, count):
        gate_part = jnp.einsum("rec,efc->ref", arrived, gate_w, preferred_element_type=jnp.float32)
        up_part = jnp.einsum("rec,efc->ref", arrived, up_w, preferred_element_type=jnp.float32)
        return jnp.concatenate([gate_part, up_part], axis=2)

    return term


def down_term(down_w, piece):
    return jnp.einsum("ref,efc->rec", piece, down_w, preferred_element_type=jnp.float32)


def activate(owned, hidden_units):
    return (jax.nn.silu(owned[:, :, :hidden_units]) * owned[:, :, hidden_units:]).astype(
        jnp.bfloat16
    )


def shards(tokens, norm_gain, route_ids, route_gates, w_gate, w_up, w_down):
    tok_rows, width_loc = tokens.shape
    top_count = route_ids.shape[1]
    exp_local = w_gate.shape[0]
    hidden_units = w_gate.shape[1]
    n_groups = lax.axis_size("ep")
    n_width = lax.axis_size("tp")
    experts = exp_local * n_groups
    capacity = max(2, (5 * tok_rows * top_count + 4 * experts - 1) // (4 * experts))
    slab_rows = n_groups * capacity
    owned_rows = slab_rows // n_width
    values = tokens.astype(jnp.float32)
    squares = lax.psum(jnp.sum(values * values, axis=1), "tp")
    inverse = lax.rsqrt(squares / (width_loc * n_width) + EPSILON)
    normed = (values * inverse[:, None] * norm_gain[None, :]).astype(jnp.bfloat16)
    flat_ids = route_ids.reshape(-1)
    onehot = (flat_ids[:, None] == jnp.arange(experts, dtype=jnp.int32)[None, :]).astype(jnp.int32)
    before = jnp.cumsum(onehot, axis=0) - onehot
    slot_of = jnp.sum(before * onehot, axis=1)
    target = (flat_ids // exp_local * capacity + slot_of) * exp_local + flat_ids % exp_local
    sources = jnp.repeat(normed, top_count, axis=0)
    buffer = jnp.zeros((slab_rows * exp_local, width_loc), jnp.bfloat16).at[target].set(sources)
    buffer = buffer.reshape(n_groups, capacity, exp_local, width_loc)
    pieces = []
    for local_idx in range(exp_local):
        single = buffer[:, :, local_idx : local_idx + 1]
        arrived = lax.all_to_all(single, "ep", split_axis=0, concat_axis=0, tiled=True).reshape(
            slab_rows, 1, width_loc
        )
        term = gate_up_term(
            arrived, w_gate[local_idx : local_idx + 1], w_up[local_idx : local_idx + 1]
        )
        owned = lax.psum_scatter(
            term(jnp.int32(0), owned_rows * lax.axis_size("tp")).astype(jnp.bfloat16),
            "tp",
            scatter_dimension=0,
            tiled=True,
        ).astype(jnp.float32)
        hidden = activate(owned, hidden_units)
        result = down_term(
            w_down[local_idx : local_idx + 1], lax.all_gather(hidden, "tp", axis=0, tiled=True)
        )
        result = result.astype(jnp.bfloat16).reshape(n_groups, capacity, 1, width_loc)
        pieces.append(lax.all_to_all(result, "ep", split_axis=0, concat_axis=0, tiled=True))
    returned = jnp.concatenate(pieces, axis=2)
    picked = returned.reshape(slab_rows * exp_local, width_loc)[target]
    weighted = (
        picked.astype(jnp.float32).reshape(tok_rows, top_count, width_loc) * route_gates[:, :, None]
    )
    return jnp.sum(weighted, axis=1).astype(jnp.bfloat16)


def slot_chunks(cuts):
    chunks = []
    for far, local_idx, counts in cuts:
        start = 0
        for count in counts:
            chunks.append((far, local_idx, start, count))
            start += count
    return chunks


def experts_kernel(
    geometry,
    tok_hbm,
    gain_hbm,
    ids_hbm,
    gates_hbm,
    wg_hbm,
    wu_hbm,
    wd_hbm,
    out_ref,
    tok_ref,
    gain_ref,
    ids_ref,
    gates_ref,
    wg,
    wu,
    wd,
    acc,
    *rest,
):
    n_groups, n_width, exp_local, chunks = geometry
    n_chunks = len(chunks)
    half = n_groups // 2
    per_chunk = 10
    bufs = [rest[per_chunk * i : per_chunk * (i + 1)] for i in range(n_chunks)]
    (in_sem, w_sem, sq_ss, sq_rs, d_ss, d_rs, p_ss, p_rs, h_ss, h_rs, r_ss, r_rs) = rest[per_chunk * n_chunks :]
    ep, tp = lax.axis_index("ep"), lax.axis_index("tp")
    tok_rows, width_loc = tok_ref.shape
    hidden_units = wg.shape[1]
    f32, bf16 = jnp.float32, jnp.bfloat16

    side, place = ep // half, lax.rem(ep, half)
    pair, core = place // 2, lax.rem(place, 2)

    def ep_peer(step):
        return {"ep": lax.rem(ep + step, n_groups), "tp": tp}

    def tp_peer(step):
        return {"ep": ep, "tp": lax.rem(tp + step, n_width)}

    def remote_peer(other):
        return {"ep": (1 - side) * half + other, "tp": tp}

    def near_peer(kind, other):
        chip = pair if kind == OWN_CHIP else 1 - pair
        return {"ep": side * half + 2 * chip + other, "tp": tp}

    barrier = pltpu.get_barrier_semaphore()
    for step in range(1, n_groups):
        pl.semaphore_signal(barrier, inc=1, device_id=ep_peer(step), device_id_type=MESH)
    for step in range(1, n_width):
        pl.semaphore_signal(barrier, inc=1, device_id=tp_peer(step), device_id_type=MESH)

    inputs = ((ids_hbm, ids_ref), (gates_hbm, gates_ref), (tok_hbm, tok_ref), (gain_hbm, gain_ref))
    input_copies = []
    for index, (src, dst) in enumerate(inputs):
        copy = pltpu.make_async_copy(src, dst, in_sem.at[index])
        copy.start()
        input_copies.append(copy)
    weight_copies = []
    for local_idx in range(exp_local):
        for which, (src, dst) in enumerate(((wg_hbm, wg), (wu_hbm, wu), (wd_hbm, wd))):
            copy = pltpu.make_async_copy(
                src.at[local_idx], dst.at[local_idx], w_sem.at[local_idx, which]
            )
            weight_copies.append(copy)

    input_copies[0].wait()
    input_copies[1].wait()
    pending = {}

    def send(src, dst, ss, rs, peer):
        copy = pltpu.make_async_remote_copy(
            src_ref=src, dst_ref=dst, send_sem=ss, recv_sem=rs, device_id=peer, device_id_type=MESH
        )
        copy.start()

    def arrival(window, sem):
        return pltpu.make_async_copy(window, window, sem)

    def spread(row):
        return jnp.broadcast_to(row, (n_groups, tok_rows))

    names = [spread(ids_ref[k : k + 1].astype(f32)) for k in range(ids_ref.shape[0])]
    weights = [spread(gates_ref[k : k + 1]) for k in range(gates_ref.shape[0])]
    earlier = (
        lax.broadcasted_iota(jnp.int32, (tok_rows, tok_rows), 0)
        < lax.broadcasted_iota(jnp.int32, (tok_rows, tok_rows), 1)
    )
    earlier = jnp.where(earlier, 1.0, 0.0).astype(bf16)
    owner = lax.broadcasted_iota(jnp.int32, (n_groups, tok_rows), 0).astype(f32)
    places, gate_of = [], []
    for local_idx in range(exp_local):
        expert = owner * float(exp_local) + float(local_idx)
        gate, named = jnp.zeros_like(owner), jnp.zeros_like(owner)
        for name, weight in zip(names, weights):
            gate = jnp.where(name == expert, weight, gate)
            named = jnp.where(name == expert, 1.0, named)
        before = jnp.dot(named.astype(bf16), earlier, preferred_element_type=f32)
        places.append(jnp.where(named > 0.0, before, -1.0))
        gate_of.append(gate)

    def grouped(values):
        low, high = values[:half], values[half:]
        mine, remote = jnp.where(side == 0, low, high), jnp.where(side == 0, high, low)
        first, second = mine[:2], mine[2:]
        chip = jnp.where(pair == 0, first, second)
        return {OWN_CHIP: chip, REMOTE: remote, NEXT_CHIP: jnp.where(pair == 0, second, first)}

    places, gate_of = [grouped(v) for v in places], [grouped(v) for v in gate_of]

    def row_of(table, i, group):
        kind, local_idx = chunks[i][:2]
        if kind != REMOTE:
            local_idx, group = group // 2, group % 2
        return table[local_idx][kind][group : group + 1]

    def expert_groups(i):
        kind, local_idx = chunks[i][:2]
        if kind == REMOTE:
            return [(local_idx, slice(0, half))]
        return [(e, slice(2 * e, 2 * e + 2)) for e in range(exp_local)]

    def hits(i, group):
        _, _, start, count = chunks[i]
        slot = lax.broadcasted_iota(jnp.int32, (count, tok_rows), 0).astype(f32) + float(start)
        return row_of(places, i, group) == slot

    sent, ready = {}, []
    input_copies[2].wait()
    for copy in weight_copies:
        copy.start()


    def keep_own(kind, source, target):
        if kind == OWN_CHIP:
            for e in range(exp_local):
                target[2 * e + core] = source[2 * e + core]

    def pick(i):
        kind, _, _, count = chunks[i]
        out_slab, in_slab = bufs[i][:2]
        picks = [jnp.where(hits(i, group), 1.0, 0.0) for group in range(half)]
        matrix = jnp.concatenate(picks, axis=0).astype(bf16)
        rows = jnp.dot(matrix, tok_ref[...], preferred_element_type=f32).astype(bf16)
        out_slab[...] = rows.reshape(half, count, width_loc)
        keep_own(kind, out_slab, in_slab)

    def exchange(kind, source, target, ss, rs):
        if kind == REMOTE:
            for step in range(half):
                other = lax.rem(place + step, half)
                send(source.at[other], target.at[place], ss, rs, remote_peer(other))
            return
        for other in (1 - core,) if kind == OWN_CHIP else (core, 1 - core):
            for e in range(exp_local):
                send(
                    source.at[2 * e + other], target.at[2 * e + core], ss, rs, near_peer(kind, other)
                )

    def window(kind, buffer):
        return buffer.at[pl.ds(0, 2)] if kind == OWN_CHIP else buffer

    def dispatch(i):
        kind = chunks[i][0]
        out_slab, in_slab = bufs[i][:2]
        if not ready:
            pl.semaphore_wait(barrier, n_groups + n_width - 2)
            ready.append(True)
        exchange(kind, out_slab, in_slab, d_ss.at[i], d_rs.at[i])
        pending[("D", i)] = arrival(window(kind, out_slab), d_ss.at[i])
        sent[i] = [arrival(window(kind, in_slab), d_rs.at[i])]

    def mixers(i):
        mixed = jnp.concatenate(
            [jnp.where(hits(i, group), row_of(gate_of, i, group), 0.0) for group in range(half)],
            axis=0,
        )
        high = mixed.astype(bf16)
        mix = bufs[i][7]
        mix[0] = high
        mix[1] = (mixed - high.astype(f32)).astype(bf16)

    def settle(i):
        pending.pop(("D", i)).wait()

    loaded = set()

    def weight_ready(local_idx, which):
        if (local_idx, which) not in loaded:
            loaded.add((local_idx, which))
            weight_copies[local_idx * 3 + which].wait()

    part_sent, hid_sent, back_sent = {}, {}, {}
    combined = []
    tile = 256 if hidden_units % 256 == 0 else 128

    def gate_up(i):
        _, _, _, count = chunks[i]
        _, in_slab, part, _, _, _, _, _, sq, sq_in = bufs[i]
        for copy in sent[i]:
            copy.wait()
        values = in_slab[...].reshape(half * count, width_loc).astype(f32)
        rows = (values * gain_ref[...]).astype(bf16)
        for local_idx, groups in expert_groups(i):
            weight_ready(local_idx, 0)
            weight_ready(local_idx, 1)
            used = rows[groups.start * count : groups.stop * count]
            for which, weight in enumerate((wg, wu)):
                for begin in range(0, hidden_units, tile):
                    block = lax.dot_general(
                        used,
                        weight[local_idx, begin : begin + tile, :],
                        (((1,), (1,)), ((), ())),
                        preferred_element_type=f32,
                    ).astype(bf16)
                    column = which * hidden_units + begin
                    part[groups, :, column : column + tile] = block.reshape(-1, count, tile)
        squares = jnp.sum(values * values, axis=1, keepdims=True)
        owned = half * count // n_width
        for who in range(n_width):
            column = jnp.broadcast_to(squares[who * owned : (who + 1) * owned], (owned, 128))
            if owned < 128:
                column = jnp.concatenate([column, jnp.zeros((128 - owned, 128), f32)], axis=0)
            sq[who] = column.T[0:8]
        for step in (2, 1, 3)[: n_width - 1]:
            dest = lax.rem(tp + step, n_width)
            send(sq.at[dest], sq_in.at[step - 1], sq_ss.at[i], sq_rs.at[i], tp_peer(step))
            send(part.at[dest], bufs[i][3].at[step - 1], p_ss.at[i], p_rs.at[i], tp_peer(step))
        pending[("Q", i)] = arrival(sq_in, sq_ss.at[i])
        pending[("P", i)] = arrival(bufs[i][3], p_ss.at[i])
        part_sent[i] = [arrival(sq_in, sq_rs.at[i]), arrival(bufs[i][3], p_rs.at[i])]

    def hidden(i):
        _, _, part, part_in, hid, _, _, _, sq, sq_in = bufs[i]
        for copy in part_sent[i]:
            copy.wait()
        owned = part.shape[1]
        total = sq[tp]
        for step in range(1, n_width):
            total = total + sq_in[step - 1]
        total = jnp.broadcast_to(total[0:1], (128, 128)).T[0:owned, 0:1]
        inverse = lax.rsqrt(total / (width_loc * n_width) + EPSILON)
        for begin in range(0, hidden_units, tile):
            sums = []
            for column in (begin, hidden_units + begin):
                value = part[tp, :, column : column + tile].astype(f32)
                for step in range(1, n_width):
                    value = value + part_in[step - 1, :, column : column + tile].astype(f32)
                sums.append(value * inverse)
            gate, up = sums
            hid[tp, :, begin : begin + tile] = (gate / (1.0 + jnp.exp(-gate)) * up).astype(bf16)
        for step in (2, 1, 3)[: n_width - 1]:
            send(hid.at[tp], hid.at[tp], h_ss.at[i], h_rs.at[i], tp_peer(step))
        pending[("H", i)] = arrival(hid.at[pl.ds(0, n_width - 1)], h_ss.at[i])
        hid_sent[i] = [arrival(hid.at[pl.ds(0, n_width - 1)], h_rs.at[i])]

    def down(i):
        kind, _, _, count = chunks[i]
        _, _, _, _, hid, result, back, _, _, _ = bufs[i]
        for copy in hid_sent[i]:
            copy.wait()
        for local_idx, groups in expert_groups(i):
            weight_ready(local_idx, 2)
            rows = hid[groups].reshape(-1, hidden_units)
            for begin in range(0, width_loc, 256):
                block = jnp.dot(
                    rows, wd[local_idx, :, begin : begin + 256], preferred_element_type=f32
                )
                result[groups, :, begin : begin + 256] = block.astype(bf16).reshape(-1, count, 256)
        exchange(kind, result, back, r_ss.at[i], r_rs.at[i])
        pending[("R", i)] = arrival(window(kind, result), r_ss.at[i])
        back_sent[i] = [arrival(window(kind, back), r_rs.at[i])]
        keep_own(kind, result, back)

    def combine(i):
        _, _, _, count = chunks[i]
        _, _, _, _, _, _, back, mix, _, _ = bufs[i]
        for copy in back_sent[i]:
            copy.wait()
        combined.append(i)
        rows = back[...].reshape(half * count, width_loc)
        value = sum(
            lax.dot_general(mix[half], rows, (((0,), (0,)), ((), ())), preferred_element_type=f32)
            for half in range(2)
        )
        if len(combined) > 1:
            value = acc[...] + value
        if len(combined) < n_chunks:
            acc[...] = value
        else:
            out_ref[...] = value.astype(bf16)

    steps = {
        "D": pick, "X": dispatch, "M": mixers, "S": settle,
         "G": gate_up, "H": hidden, "W": down, "C": combine
    }
    input_copies[3].wait()
    for word in ORDER:
        steps[word[0]](int(word[1:]))
    for copy in pending.values():
        copy.wait()


ORDER = (
    "D0", "X0", "D4", "X4", "D5", "X5", "D1", "X1", "D2", "X2", "D3", "X3",
    "M0", "M1", "M2", "M3", "M4", "M5", "G4", "G0", "H4", "G5", "H0", "W4",
    "W0", "G1", "H1", "H5", "G2", "W1", "W5", "H2", "G3", "W2", "H3", "W3",
    "C4", "C5", "C0", "C1", "C2", "C3",
)


def kernel_shards(
    cuts, tokens, norm_gain, route_ids, route_gates, w_gate, w_up, w_down
):
    tok_rows, width_loc = tokens.shape
    exp_local, hidden_units, _ = w_gate.shape
    n_groups, n_width = lax.axis_size("ep"), lax.axis_size("tp")
    chunks = slot_chunks(cuts)
    half = n_groups // 2
    f32, bf16 = jnp.float32, jnp.bfloat16
    per_chunk = []
    for _, _, _, count in chunks:
        rows = half * count
        per_chunk += [
            pltpu.VMEM((half, count, width_loc), bf16),
            pltpu.VMEM((half, count, width_loc), bf16),
            pltpu.VMEM((n_width, rows // n_width, 2 * hidden_units), bf16),
            pltpu.VMEM((n_width - 1, rows // n_width, 2 * hidden_units), bf16),
            pltpu.VMEM((n_width, rows // n_width, hidden_units), bf16),
            pltpu.VMEM((half, count, width_loc), bf16),
            pltpu.VMEM((half, count, width_loc), bf16),
            pltpu.VMEM((2, rows, tok_rows), bf16),
            pltpu.VMEM((n_width, 8, 128), f32),
            pltpu.VMEM((n_width - 1, 8, 128), f32),
        ]
    operands = (
        tokens, norm_gain.reshape(1, width_loc), route_ids.T, route_gates.T, w_gate, w_up, w_down
    )
    n_chunks = len(chunks)
    sems = [pltpu.SemaphoreType.DMA((4,)), pltpu.SemaphoreType.DMA((exp_local, 3))]
    sems += [pltpu.SemaphoreType.DMA((n_chunks,))] * 10
    anywhere = pl.BlockSpec(memory_space=pl.ANY)
    return pl.pallas_call(
        functools.partial(experts_kernel, (n_groups, n_width, exp_local, chunks)),
        out_shape=jax.ShapeDtypeStruct((tok_rows, width_loc), bf16),
        in_specs=[anywhere] * 7,
        out_specs=pl.BlockSpec(memory_space=pltpu.VMEM),
        scratch_shapes=[
            pltpu.VMEM(tokens.shape, bf16),
            pltpu.VMEM((1, width_loc), f32),
            pltpu.VMEM(route_ids.shape[::-1], jnp.int32),
            pltpu.VMEM(route_gates.shape[::-1], f32),
            pltpu.VMEM(w_gate.shape, bf16),
            pltpu.VMEM(w_up.shape, bf16),
            pltpu.VMEM(w_down.shape, bf16),
            pltpu.VMEM((tok_rows, width_loc), f32),
            *per_chunk,
            *sems,
        ],
        compiler_params=pltpu.CompilerParams(
            collective_id=0, has_side_effects=True, vmem_limit_bytes=40 * 1024 * 1024
        ),
    )(*[pltpu.with_memory_space_constraint(array, pltpu.HBM) for array in operands])


def plan(capacity):
    if capacity % 8:
        return None
    return ((1, 0, (16, 24)), (1, 1, (24, 16)), (0, 0, (40,)), (2, 0, (40,)))


def solution(mesh):
    placed = (
        P("ep", "tp"),
        P("tp"),
        P("ep", None),
        P("ep", None),
        P("ep", None, "tp"),
        P("ep", None, "tp"),
        P("ep", None, "tp"),
    )
    n_groups, n_width = mesh.shape["ep"], mesh.shape["tp"]

    def body(tokens, norm_gain, route_ids, route_gates, w_gate, w_up, w_down):
        experts = w_gate.shape[0] * n_groups
        tok_rows, width_loc = tokens.shape
        top_count = route_ids.shape[1]
        capacity = max(2, (5 * tok_rows * top_count + 4 * experts - 1) // (4 * experts))
        cuts = plan(capacity)
        arrays = (tokens, norm_gain, route_ids, route_gates, w_gate, w_up, w_down)
        if cuts is None or n_groups != 8 or n_width != 4 or width_loc % 256 or tok_rows % 128:
            return shards(*arrays)
        return kernel_shards(cuts, *arrays)

    return jax.shard_map(
        body, mesh=mesh, in_specs=placed, out_specs=P("ep", "tp"), check_vma=False
    )
```

```python
import functools

import jax
import jax.numpy as jnp
from jax import lax
from jax.experimental import pallas as pl
from jax.experimental.pallas import tpu as pltpu
from jax.sharding import PartitionSpec as P

EPSILON = 1e-06
MESH = pl.DeviceIdType.MESH
OWN_CHIP, REMOTE, NEXT_CHIP = range(3)


def gate_up_term(arrived, gate_w, up_w):

    def term(start, count):
        gate_part = jnp.einsum("rec,efc->ref", arrived, gate_w, preferred_element_type=jnp.float32)
        up_part = jnp.einsum("rec,efc->ref", arrived, up_w, preferred_element_type=jnp.float32)
        return jnp.concatenate([gate_part, up_part], axis=2)

    return term


def down_term(down_w, piece):
    return jnp.einsum("ref,efc->rec", piece, down_w, preferred_element_type=jnp.float32)


def activate(owned, hidden_units):
    return (jax.nn.silu(owned[:, :, :hidden_units]) * owned[:, :, hidden_units:]).astype(
        jnp.bfloat16
    )


def shards(tokens, norm_gain, route_ids, route_gates, w_gate, w_up, w_down):
    tok_rows, width_loc = tokens.shape
    top_count = route_ids.shape[1]
    exp_local = w_gate.shape[0]
    hidden_units = w_gate.shape[1]
    n_groups = lax.axis_size("ep")
    n_width = lax.axis_size("tp")
    experts = exp_local * n_groups
    capacity = max(2, (5 * tok_rows * top_count + 4 * experts - 1) // (4 * experts))
    slab_rows = n_groups * capacity
    owned_rows = slab_rows // n_width
    values = tokens.astype(jnp.float32)
    squares = lax.psum(jnp.sum(values * values, axis=1), "tp")
    inverse = lax.rsqrt(squares / (width_loc * n_width) + EPSILON)
    normed = (values * inverse[:, None] * norm_gain[None, :]).astype(jnp.bfloat16)
    flat_ids = route_ids.reshape(-1)
    onehot = (flat_ids[:, None] == jnp.arange(experts, dtype=jnp.int32)[None, :]).astype(jnp.int32)
    before = jnp.cumsum(onehot, axis=0) - onehot
    slot_of = jnp.sum(before * onehot, axis=1)
    target = (flat_ids // exp_local * capacity + slot_of) * exp_local + flat_ids % exp_local
    sources = jnp.repeat(normed, top_count, axis=0)
    buffer = jnp.zeros((slab_rows * exp_local, width_loc), jnp.bfloat16).at[target].set(sources)
    buffer = buffer.reshape(n_groups, capacity, exp_local, width_loc)
    pieces = []
    for local_idx in range(exp_local):
        single = buffer[:, :, local_idx : local_idx + 1]
        arrived = lax.all_to_all(single, "ep", split_axis=0, concat_axis=0, tiled=True).reshape(
            slab_rows, 1, width_loc
        )
        term = gate_up_term(
            arrived, w_gate[local_idx : local_idx + 1], w_up[local_idx : local_idx + 1]
        )
        owned = lax.psum_scatter(
            term(jnp.int32(0), owned_rows * lax.axis_size("tp")).astype(jnp.bfloat16),
            "tp",
            scatter_dimension=0,
            tiled=True,
        ).astype(jnp.float32)
        hidden = activate(owned, hidden_units)
        result = down_term(
            w_down[local_idx : local_idx + 1], lax.all_gather(hidden, "tp", axis=0, tiled=True)
        )
        result = result.astype(jnp.bfloat16).reshape(n_groups, capacity, 1, width_loc)
        pieces.append(lax.all_to_all(result, "ep", split_axis=0, concat_axis=0, tiled=True))
    returned = jnp.concatenate(pieces, axis=2)
    picked = returned.reshape(slab_rows * exp_local, width_loc)[target]
    weighted = (
        picked.astype(jnp.float32).reshape(tok_rows, top_count, width_loc) * route_gates[:, :, None]
    )
    return jnp.sum(weighted, axis=1).astype(jnp.bfloat16)


def slot_chunks(cuts):
    chunks = []
    for far, local_idx, counts in cuts:
        start = 0
        for count in counts:
            chunks.append((far, local_idx, start, count))
            start += count
    return chunks


def experts_kernel(
    geometry,
    tok_hbm,
    gain_hbm,
    ids_hbm,
    gates_hbm,
    wg_hbm,
    wu_hbm,
    wd_hbm,
    out_ref,
    tok_ref,
    gain_ref,
    ids_ref,
    gates_ref,
    wg,
    wu,
    wd,
    acc,
    *rest,
):
    n_groups, n_width, exp_local, chunks = geometry
    n_chunks = len(chunks)
    half = n_groups // 2
    per_chunk = 10
    bufs = [rest[per_chunk * i : per_chunk * (i + 1)] for i in range(n_chunks)]
    (in_sem, w_sem, sq_ss, sq_rs, d_ss, d_rs, p_ss, p_rs, h_ss, h_rs, r_ss, r_rs) = rest[per_chunk * n_chunks :]
    ep, tp = lax.axis_index("ep"), lax.axis_index("tp")
    tok_rows, width_loc = tok_ref.shape
    hidden_units = wg.shape[1]
    f32, bf16 = jnp.float32, jnp.bfloat16

    side, place = ep // half, lax.rem(ep, half)
    pair, core = place // 2, lax.rem(place, 2)

    def ep_peer(step):
        return {"ep": lax.rem(ep + step, n_groups), "tp": tp}

    def tp_peer(step):
        return {"ep": ep, "tp": lax.rem(tp + step, n_width)}

    def remote_peer(other):
        return {"ep": (1 - side) * half + other, "tp": tp}

    def near_peer(kind, other):
        chip = pair if kind == OWN_CHIP else 1 - pair
        return {"ep": side * half + 2 * chip + other, "tp": tp}

    barrier = pltpu.get_barrier_semaphore()
    for step in range(1, n_groups):
        pl.semaphore_signal(barrier, inc=1, device_id=ep_peer(step), device_id_type=MESH)
    for step in range(1, n_width):
        pl.semaphore_signal(barrier, inc=1, device_id=tp_peer(step), device_id_type=MESH)

    inputs = ((ids_hbm, ids_ref), (gates_hbm, gates_ref), (tok_hbm, tok_ref), (gain_hbm, gain_ref))
    input_copies = []
    for index, (src, dst) in enumerate(inputs):
        copy = pltpu.make_async_copy(src, dst, in_sem.at[index])
        copy.start()
        input_copies.append(copy)
    weight_copies = []
    for local_idx in range(exp_local):
        for which, (src, dst) in enumerate(((wg_hbm, wg), (wu_hbm, wu), (wd_hbm, wd))):
            copy = pltpu.make_async_copy(
                src.at[local_idx], dst.at[local_idx], w_sem.at[local_idx, which]
            )
            weight_copies.append(copy)

    input_copies[0].wait()
    input_copies[1].wait()
    pending = {}

    def send(src, dst, ss, rs, peer):
        copy = pltpu.make_async_remote_copy(
            src_ref=src, dst_ref=dst, send_sem=ss, recv_sem=rs, device_id=peer, device_id_type=MESH
        )
        copy.start()

    def arrival(window, sem):
        return pltpu.make_async_copy(window, window, sem)

    def spread(row):
        return jnp.broadcast_to(row, (n_groups, tok_rows))

    names = [spread(ids_ref[k : k + 1].astype(f32)) for k in range(ids_ref.shape[0])]
    weights = [spread(gates_ref[k : k + 1]) for k in range(gates_ref.shape[0])]
    earlier = (
        lax.broadcasted_iota(jnp.int32, (tok_rows, tok_rows), 0)
        < lax.broadcasted_iota(jnp.int32, (tok_rows, tok_rows), 1)
    )
    earlier = jnp.where(earlier, 1.0, 0.0).astype(bf16)
    owner = lax.broadcasted_iota(jnp.int32, (n_groups, tok_rows), 0).astype(f32)
    places, gate_of = [], []
    for local_idx in range(exp_local):
        expert = owner * float(exp_local) + float(local_idx)
        gate, named = jnp.zeros_like(owner), jnp.zeros_like(owner)
        for name, weight in zip(names, weights):
            gate = jnp.where(name == expert, weight, gate)
            named = jnp.where(name == expert, 1.0, named)
        before = jnp.dot(named.astype(bf16), earlier, preferred_element_type=f32)
        places.append(jnp.where(named > 0.0, before, -1.0))
        gate_of.append(gate)

    def grouped(values):
        low, high = values[:half], values[half:]
        mine, remote = jnp.where(side == 0, low, high), jnp.where(side == 0, high, low)
        first, second = mine[:2], mine[2:]
        chip = jnp.where(pair == 0, first, second)
        return {OWN_CHIP: chip, REMOTE: remote, NEXT_CHIP: jnp.where(pair == 0, second, first)}

    places, gate_of = [grouped(v) for v in places], [grouped(v) for v in gate_of]

    def row_of(table, i, group):
        kind, local_idx = chunks[i][:2]
        if kind != REMOTE:
            local_idx, group = group // 2, group % 2
        return table[local_idx][kind][group : group + 1]

    def expert_groups(i):
        kind, local_idx = chunks[i][:2]
        if kind == REMOTE:
            return [(local_idx, slice(0, half))]
        return [(e, slice(2 * e, 2 * e + 2)) for e in range(exp_local)]

    def hits(i, group):
        _, _, start, count = chunks[i]
        slot = lax.broadcasted_iota(jnp.int32, (count, tok_rows), 0).astype(f32) + float(start)
        return row_of(places, i, group) == slot

    sent, ready = {}, []
    input_copies[2].wait()
    for copy in weight_copies:
        copy.start()


    def keep_own(kind, source, target):
        if kind == OWN_CHIP:
            for e in range(exp_local):
                target[2 * e + core] = source[2 * e + core]

    def pick(i):
        kind, _, _, count = chunks[i]
        out_slab, in_slab = bufs[i][:2]
        picks = [jnp.where(hits(i, group), 1.0, 0.0) for group in range(half)]
        matrix = jnp.concatenate(picks, axis=0).astype(bf16)
        rows = jnp.dot(matrix, tok_ref[...], preferred_element_type=f32).astype(bf16)
        out_slab[...] = rows.reshape(half, count, width_loc)
        keep_own(kind, out_slab, in_slab)

    def exchange(kind, source, target, ss, rs):
        if kind == REMOTE:
            for step in range(half):
                other = lax.rem(place + step, half)
                send(source.at[other], target.at[place], ss, rs, remote_peer(other))
            return
        for other in (1 - core,) if kind == OWN_CHIP else (core, 1 - core):
            for e in range(exp_local):
                send(
                    source.at[2 * e + other], target.at[2 * e + core], ss, rs, near_peer(kind, other)
                )

    def window(kind, buffer):
        return buffer.at[pl.ds(0, 2)] if kind == OWN_CHIP else buffer

    def dispatch(i):
        kind = chunks[i][0]
        out_slab, in_slab = bufs[i][:2]
        if not ready:
            pl.semaphore_wait(barrier, n_groups + n_width - 2)
            ready.append(True)
        exchange(kind, out_slab, in_slab, d_ss.at[i], d_rs.at[i])
        register(i)

    def register(i):
        kind = chunks[i][0]
        pending[("D", i)] = arrival(window(kind, bufs[i][0]), d_ss.at[i])
        sent[i] = [arrival(window(kind, bufs[i][1]), d_rs.at[i])]

    def from_ends(i):
        register(i)
        out_slab, in_slab = bufs[i][:2]

        def start():
            exchange(chunks[i][0], out_slab, in_slab, d_ss.at[i], d_rs.at[i])

        pl.when(pair == side)(start)

    def from_middle(i):
        out_slab, in_slab = bufs[i][:2]

        def start():
            exchange(chunks[i][0], out_slab, in_slab, d_ss.at[i], d_rs.at[i])

        pl.when(pair != side)(start)

    def mixers(i):
        mixed = jnp.concatenate(
            [jnp.where(hits(i, group), row_of(gate_of, i, group), 0.0) for group in range(half)],
            axis=0,
        )
        high = mixed.astype(bf16)
        mix = bufs[i][7]
        mix[0] = high
        mix[1] = (mixed - high.astype(f32)).astype(bf16)

    def settle(i):
        pending.pop(("D", i)).wait()

    loaded = set()

    def weight_ready(local_idx, which):
        if (local_idx, which) not in loaded:
            loaded.add((local_idx, which))
            weight_copies[local_idx * 3 + which].wait()

    part_sent, hid_sent, back_sent = {}, {}, {}
    combined = []
    tile = 256 if hidden_units % 256 == 0 else 128

    def gate_up(i):
        _, _, _, count = chunks[i]
        _, in_slab, part, _, _, _, _, _, sq, sq_in = bufs[i]
        for copy in sent[i]:
            copy.wait()
        values = in_slab[...].reshape(half * count, width_loc).astype(f32)
        rows = (values * gain_ref[...]).astype(bf16)
        for local_idx, groups in expert_groups(i):
            weight_ready(local_idx, 0)
            weight_ready(local_idx, 1)
            used = rows[groups.start * count : groups.stop * count]
            for which, weight in enumerate((wg, wu)):
                for begin in range(0, hidden_units, tile):
                    block = lax.dot_general(
                        used,
                        weight[local_idx, begin : begin + tile, :],
                        (((1,), (1,)), ((), ())),
                        preferred_element_type=f32,
                    ).astype(bf16)
                    column = which * hidden_units + begin
                    part[groups, :, column : column + tile] = block.reshape(-1, count, tile)
        squares = jnp.sum(values * values, axis=1, keepdims=True)
        owned = half * count // n_width
        for who in range(n_width):
            column = jnp.broadcast_to(squares[who * owned : (who + 1) * owned], (owned, 128))
            if owned < 128:
                column = jnp.concatenate([column, jnp.zeros((128 - owned, 128), f32)], axis=0)
            sq[who] = column.T[0:8]
        for step in (2, 1, 3)[: n_width - 1]:
            dest = lax.rem(tp + step, n_width)
            send(sq.at[dest], sq_in.at[step - 1], sq_ss.at[i], sq_rs.at[i], tp_peer(step))
            send(part.at[dest], bufs[i][3].at[step - 1], p_ss.at[i], p_rs.at[i], tp_peer(step))
        pending[("Q", i)] = arrival(sq_in, sq_ss.at[i])
        pending[("P", i)] = arrival(bufs[i][3], p_ss.at[i])
        part_sent[i] = [arrival(sq_in, sq_rs.at[i]), arrival(bufs[i][3], p_rs.at[i])]

    def hidden(i):
        _, _, part, part_in, hid, _, _, _, sq, sq_in = bufs[i]
        for copy in part_sent[i]:
            copy.wait()
        owned = part.shape[1]
        total = sq[tp]
        for step in range(1, n_width):
            total = total + sq_in[step - 1]
        total = jnp.broadcast_to(total[0:1], (128, 128)).T[0:owned, 0:1]
        inverse = lax.rsqrt(total / (width_loc * n_width) + EPSILON)
        for begin in range(0, hidden_units, tile):
            sums = []
            for column in (begin, hidden_units + begin):
                value = part[tp, :, column : column + tile].astype(f32)
                for step in range(1, n_width):
                    value = value + part_in[step - 1, :, column : column + tile].astype(f32)
                sums.append(value * inverse)
            gate, up = sums
            hid[tp, :, begin : begin + tile] = (gate / (1.0 + jnp.exp(-gate)) * up).astype(bf16)
        for step in (2, 1, 3)[: n_width - 1]:
            send(hid.at[tp], hid.at[tp], h_ss.at[i], h_rs.at[i], tp_peer(step))
        pending[("H", i)] = arrival(hid.at[pl.ds(0, n_width - 1)], h_ss.at[i])
        hid_sent[i] = [arrival(hid.at[pl.ds(0, n_width - 1)], h_rs.at[i])]

    def down(i):
        kind, _, _, count = chunks[i]
        _, _, _, _, hid, result, back, _, _, _ = bufs[i]
        for copy in hid_sent[i]:
            copy.wait()
        for local_idx, groups in expert_groups(i):
            weight_ready(local_idx, 2)
            rows = hid[groups].reshape(-1, hidden_units)
            for begin in range(0, width_loc, 256):
                block = jnp.dot(
                    rows, wd[local_idx, :, begin : begin + 256], preferred_element_type=f32
                )
                result[groups, :, begin : begin + 256] = block.astype(bf16).reshape(-1, count, 256)
        exchange(kind, result, back, r_ss.at[i], r_rs.at[i])
        pending[("R", i)] = arrival(window(kind, result), r_ss.at[i])
        back_sent[i] = [arrival(window(kind, back), r_rs.at[i])]
        keep_own(kind, result, back)

    def combine(i):
        _, _, _, count = chunks[i]
        _, _, _, _, _, _, back, mix, _, _ = bufs[i]
        for copy in back_sent[i]:
            copy.wait()
        combined.append(i)
        rows = back[...].reshape(half * count, width_loc)
        value = sum(
            lax.dot_general(mix[half], rows, (((0,), (0,)), ((), ())), preferred_element_type=f32)
            for half in range(2)
        )
        if len(combined) > 1:
            value = acc[...] + value
        if len(combined) < n_chunks:
            acc[...] = value
        else:
            out_ref[...] = value.astype(bf16)

    steps = {
        "D": pick, "X": dispatch, "E": from_ends, "N": from_middle, "M": mixers, "S": settle,
         "G": gate_up, "H": hidden, "W": down, "C": combine
    }
    input_copies[3].wait()
    for word in ORDER:
        steps[word[0]](int(word[1:]))
    for copy in pending.values():
        copy.wait()


ORDER = (
    "D0", "X0", "D4", "X4", "D5", "X5", "D1", "X1", "D2", "E2", "D3", "E3",
    "M0", "M1", "M2", "M3", "M4", "M5", "G4", "G0", "N2", "H4", "N3", "G5",
    "H0", "G1", "W4", "W0", "H1", "H5", "G2", "W1", "W5", "H2", "G3", "W2",
    "H3", "W3", "C4", "C5", "C0", "C1", "C2", "C3",
)


def kernel_shards(
    cuts, tokens, norm_gain, route_ids, route_gates, w_gate, w_up, w_down
):
    tok_rows, width_loc = tokens.shape
    exp_local, hidden_units, _ = w_gate.shape
    n_groups, n_width = lax.axis_size("ep"), lax.axis_size("tp")
    chunks = slot_chunks(cuts)
    half = n_groups // 2
    f32, bf16 = jnp.float32, jnp.bfloat16
    per_chunk = []
    for _, _, _, count in chunks:
        rows = half * count
        per_chunk += [
            pltpu.VMEM((half, count, width_loc), bf16),
            pltpu.VMEM((half, count, width_loc), bf16),
            pltpu.VMEM((n_width, rows // n_width, 2 * hidden_units), bf16),
            pltpu.VMEM((n_width - 1, rows // n_width, 2 * hidden_units), bf16),
            pltpu.VMEM((n_width, rows // n_width, hidden_units), bf16),
            pltpu.VMEM((half, count, width_loc), bf16),
            pltpu.VMEM((half, count, width_loc), bf16),
            pltpu.VMEM((2, rows, tok_rows), bf16),
            pltpu.VMEM((n_width, 8, 128), f32),
            pltpu.VMEM((n_width - 1, 8, 128), f32),
        ]
    operands = (
        tokens, norm_gain.reshape(1, width_loc), route_ids.T, route_gates.T, w_gate, w_up, w_down
    )
    n_chunks = len(chunks)
    sems = [pltpu.SemaphoreType.DMA((4,)), pltpu.SemaphoreType.DMA((exp_local, 3))]
    sems += [pltpu.SemaphoreType.DMA((n_chunks,))] * 10
    anywhere = pl.BlockSpec(memory_space=pl.ANY)
    return pl.pallas_call(
        functools.partial(experts_kernel, (n_groups, n_width, exp_local, chunks)),
        out_shape=jax.ShapeDtypeStruct((tok_rows, width_loc), bf16),
        in_specs=[anywhere] * 7,
        out_specs=pl.BlockSpec(memory_space=pltpu.VMEM),
        scratch_shapes=[
            pltpu.VMEM(tokens.shape, bf16),
            pltpu.VMEM((1, width_loc), f32),
            pltpu.VMEM(route_ids.shape[::-1], jnp.int32),
            pltpu.VMEM(route_gates.shape[::-1], f32),
            pltpu.VMEM(w_gate.shape, bf16),
            pltpu.VMEM(w_up.shape, bf16),
            pltpu.VMEM(w_down.shape, bf16),
            pltpu.VMEM((tok_rows, width_loc), f32),
            *per_chunk,
            *sems,
        ],
        compiler_params=pltpu.CompilerParams(
            collective_id=0, has_side_effects=True, vmem_limit_bytes=40 * 1024 * 1024
        ),
    )(*[pltpu.with_memory_space_constraint(array, pltpu.HBM) for array in operands])


def plan(capacity):
    if capacity % 8 or capacity < 24:
        return None
    large = capacity // 16 * 8 + 8
    pieces = (large, capacity - large)
    return (
        (REMOTE, 0, pieces),
        (REMOTE, 1, pieces),
        (OWN_CHIP, 0, (capacity,)),
        (NEXT_CHIP, 0, (capacity,)),
    )


def solution(mesh):
    placed = (
        P("ep", "tp"),
        P("tp"),
        P("ep", None),
        P("ep", None),
        P("ep", None, "tp"),
        P("ep", None, "tp"),
        P("ep", None, "tp"),
    )
    n_groups, n_width = mesh.shape["ep"], mesh.shape["tp"]

    def body(tokens, norm_gain, route_ids, route_gates, w_gate, w_up, w_down):
        experts = w_gate.shape[0] * n_groups
        tok_rows, width_loc = tokens.shape
        top_count = route_ids.shape[1]
        capacity = max(2, (5 * tok_rows * top_count + 4 * experts - 1) // (4 * experts))
        cuts = plan(capacity)
        arrays = (tokens, norm_gain, route_ids, route_gates, w_gate, w_up, w_down)
        fits = n_groups == 8 and n_width == 4 and w_gate.shape[0] == 2 and capacity <= 128
        if cuts is None or not fits or width_loc % 256 or tok_rows % 128:
            return shards(*arrays)
        return kernel_shards(cuts, *arrays)

    return jax.shard_map(
        body, mesh=mesh, in_specs=placed, out_specs=P("ep", "tp"), check_vma=False
    )
```

```python
import functools

import jax
import jax.numpy as jnp
from jax import lax
from jax.experimental import pallas as pl
from jax.experimental.pallas import tpu as pltpu
from jax.sharding import PartitionSpec as P

EPSILON = 1e-06
MESH = pl.DeviceIdType.MESH
OWN_CHIP, REMOTE, NEXT_CHIP = range(3)


def gate_up_term(arrived, gate_w, up_w):

    def term(start, count):
        gate_part = jnp.einsum("rec,efc->ref", arrived, gate_w, preferred_element_type=jnp.float32)
        up_part = jnp.einsum("rec,efc->ref", arrived, up_w, preferred_element_type=jnp.float32)
        return jnp.concatenate([gate_part, up_part], axis=2)

    return term


def down_term(down_w, piece):
    return jnp.einsum("ref,efc->rec", piece, down_w, preferred_element_type=jnp.float32)


def activate(owned, hidden_units):
    return (jax.nn.silu(owned[:, :, :hidden_units]) * owned[:, :, hidden_units:]).astype(
        jnp.bfloat16
    )


def shards(tokens, norm_gain, route_ids, route_gates, w_gate, w_up, w_down):
    tok_rows, width_loc = tokens.shape
    top_count = route_ids.shape[1]
    exp_local = w_gate.shape[0]
    hidden_units = w_gate.shape[1]
    n_groups = lax.axis_size("ep")
    n_width = lax.axis_size("tp")
    experts = exp_local * n_groups
    capacity = max(2, (5 * tok_rows * top_count + 4 * experts - 1) // (4 * experts))
    slab_rows = n_groups * capacity
    owned_rows = slab_rows // n_width
    values = tokens.astype(jnp.float32)
    squares = lax.psum(jnp.sum(values * values, axis=1), "tp")
    inverse = lax.rsqrt(squares / (width_loc * n_width) + EPSILON)
    normed = (values * inverse[:, None] * norm_gain[None, :]).astype(jnp.bfloat16)
    flat_ids = route_ids.reshape(-1)
    onehot = (flat_ids[:, None] == jnp.arange(experts, dtype=jnp.int32)[None, :]).astype(jnp.int32)
    before = jnp.cumsum(onehot, axis=0) - onehot
    slot_of = jnp.sum(before * onehot, axis=1)
    target = (flat_ids // exp_local * capacity + slot_of) * exp_local + flat_ids % exp_local
    sources = jnp.repeat(normed, top_count, axis=0)
    buffer = jnp.zeros((slab_rows * exp_local, width_loc), jnp.bfloat16).at[target].set(sources)
    buffer = buffer.reshape(n_groups, capacity, exp_local, width_loc)
    pieces = []
    for local_idx in range(exp_local):
        single = buffer[:, :, local_idx : local_idx + 1]
        arrived = lax.all_to_all(single, "ep", split_axis=0, concat_axis=0, tiled=True).reshape(
            slab_rows, 1, width_loc
        )
        term = gate_up_term(
            arrived, w_gate[local_idx : local_idx + 1], w_up[local_idx : local_idx + 1]
        )
        owned = lax.psum_scatter(
            term(jnp.int32(0), owned_rows * lax.axis_size("tp")).astype(jnp.bfloat16),
            "tp",
            scatter_dimension=0,
            tiled=True,
        ).astype(jnp.float32)
        hidden = activate(owned, hidden_units)
        result = down_term(
            w_down[local_idx : local_idx + 1], lax.all_gather(hidden, "tp", axis=0, tiled=True)
        )
        result = result.astype(jnp.bfloat16).reshape(n_groups, capacity, 1, width_loc)
        pieces.append(lax.all_to_all(result, "ep", split_axis=0, concat_axis=0, tiled=True))
    returned = jnp.concatenate(pieces, axis=2)
    picked = returned.reshape(slab_rows * exp_local, width_loc)[target]
    weighted = (
        picked.astype(jnp.float32).reshape(tok_rows, top_count, width_loc) * route_gates[:, :, None]
    )
    return jnp.sum(weighted, axis=1).astype(jnp.bfloat16)


def slot_chunks(cuts):
    chunks = []
    for far, local_idx, counts in cuts:
        start = 0
        for count in counts:
            chunks.append((far, local_idx, start, count))
            start += count
    return chunks


def experts_kernel(
    geometry,
    tok_hbm,
    gain_hbm,
    ids_hbm,
    gates_hbm,
    wg_hbm,
    wu_hbm,
    wd_hbm,
    out_ref,
    tok_ref,
    gain_ref,
    ids_ref,
    gates_ref,
    wg,
    wu,
    wd,
    acc,
    *rest,
):
    n_groups, n_width, exp_local, chunks = geometry
    n_chunks = len(chunks)
    half = n_groups // 2
    per_chunk = 10
    bufs = [rest[per_chunk * i : per_chunk * (i + 1)] for i in range(n_chunks)]
    (in_sem, w_sem, sq_ss, sq_rs, d_ss, d_rs, p_ss, p_rs, h_rs, r_rs) = rest[per_chunk * n_chunks :]
    ep, tp = lax.axis_index("ep"), lax.axis_index("tp")
    tok_rows, width_loc = tok_ref.shape
    hidden_units = wg.shape[1]
    f32, bf16 = jnp.float32, jnp.bfloat16

    side, place = ep // half, lax.rem(ep, half)
    pair, core = place // 2, lax.rem(place, 2)

    def ep_peer(step):
        return {"ep": lax.rem(ep + step, n_groups), "tp": tp}

    def tp_peer(step):
        return {"ep": ep, "tp": lax.rem(tp + step, n_width)}

    def remote_peer(other):
        return {"ep": (1 - side) * half + other, "tp": tp}

    def near_peer(kind, other):
        chip = pair if kind == OWN_CHIP else 1 - pair
        return {"ep": side * half + 2 * chip + other, "tp": tp}

    barrier = pltpu.get_barrier_semaphore()
    for step in range(1, n_groups):
        pl.semaphore_signal(barrier, inc=1, device_id=ep_peer(step), device_id_type=MESH)
    for step in range(1, n_width):
        pl.semaphore_signal(barrier, inc=1, device_id=tp_peer(step), device_id_type=MESH)

    inputs = ((ids_hbm, ids_ref), (gates_hbm, gates_ref), (tok_hbm, tok_ref), (gain_hbm, gain_ref))
    input_copies = []
    for index, (src, dst) in enumerate(inputs):
        copy = pltpu.make_async_copy(src, dst, in_sem.at[index])
        copy.start()
        input_copies.append(copy)
    weight_copies = []
    for local_idx in range(exp_local):
        for which, (src, dst) in enumerate(((wg_hbm, wg), (wu_hbm, wu), (wd_hbm, wd))):
            copy = pltpu.make_async_copy(
                src.at[local_idx], dst.at[local_idx], w_sem.at[local_idx, which]
            )
            weight_copies.append(copy)

    input_copies[0].wait()
    input_copies[1].wait()
    pending = {}

    def send(src, dst, ss, rs, peer):
        copy = pltpu.make_async_remote_copy(
            src_ref=src, dst_ref=dst, send_sem=ss, recv_sem=rs, device_id=peer, device_id_type=MESH
        )
        copy.start()

    def arrival(window, sem):
        return pltpu.make_async_copy(window, window, sem)

    def spread(row):
        return jnp.broadcast_to(row, (n_groups, tok_rows))

    names = [spread(ids_ref[k : k + 1].astype(f32)) for k in range(ids_ref.shape[0])]
    weights = [spread(gates_ref[k : k + 1]) for k in range(gates_ref.shape[0])]
    earlier = (
        lax.broadcasted_iota(jnp.int32, (tok_rows, tok_rows), 0)
        < lax.broadcasted_iota(jnp.int32, (tok_rows, tok_rows), 1)
    )
    earlier = jnp.where(earlier, 1.0, 0.0).astype(bf16)
    owner = lax.broadcasted_iota(jnp.int32, (n_groups, tok_rows), 0).astype(f32)
    places, gate_of = [], []
    for local_idx in range(exp_local):
        expert = owner * float(exp_local) + float(local_idx)
        gate, named = jnp.zeros_like(owner), jnp.zeros_like(owner)
        for name, weight in zip(names, weights):
            gate = jnp.where(name == expert, weight, gate)
            named = jnp.where(name == expert, 1.0, named)
        before = jnp.dot(named.astype(bf16), earlier, preferred_element_type=f32)
        places.append(jnp.where(named > 0.0, before, -1.0))
        gate_of.append(gate)

    def grouped(values):
        low, high = values[:half], values[half:]
        mine, remote = jnp.where(side == 0, low, high), jnp.where(side == 0, high, low)
        first, second = mine[:2], mine[2:]
        chip = jnp.where(pair == 0, first, second)
        return {OWN_CHIP: chip, REMOTE: remote, NEXT_CHIP: jnp.where(pair == 0, second, first)}

    places, gate_of = [grouped(v) for v in places], [grouped(v) for v in gate_of]

    def row_of(table, i, group):
        kind, local_idx = chunks[i][:2]
        if kind != REMOTE:
            local_idx, group = group // 2, group % 2
        return table[local_idx][kind][group : group + 1]

    def expert_groups(i):
        kind, local_idx = chunks[i][:2]
        if kind == REMOTE:
            return [(local_idx, slice(0, half))]
        return [(e, slice(2 * e, 2 * e + 2)) for e in range(exp_local)]

    def hits(i, group):
        _, _, start, count = chunks[i]
        slot = lax.broadcasted_iota(jnp.int32, (count, tok_rows), 0).astype(f32) + float(start)
        return row_of(places, i, group) == slot

    sent, ready = {}, []
    input_copies[2].wait()
    for copy in weight_copies:
        copy.start()


    def keep_own(kind, source, target):
        if kind == OWN_CHIP:
            for e in range(exp_local):
                target[2 * e + core] = source[2 * e + core]

    def pick(i):
        kind, _, _, count = chunks[i]
        out_slab, in_slab = bufs[i][:2]
        picks = [jnp.where(hits(i, group), 1.0, 0.0) for group in range(half)]
        matrix = jnp.concatenate(picks, axis=0).astype(bf16)
        rows = jnp.dot(matrix, tok_ref[...], preferred_element_type=f32).astype(bf16)
        out_slab[...] = rows.reshape(half, count, width_loc)
        keep_own(kind, out_slab, in_slab)

    def exchange(kind, source, target, ss, rs):
        if kind == REMOTE:
            for step in range(half):
                other = lax.rem(place + step, half)
                send(source.at[other], target.at[place], ss, rs, remote_peer(other))
            return
        for other in (1 - core,) if kind == OWN_CHIP else (core, 1 - core):
            for e in range(exp_local):
                send(
                    source.at[2 * e + other], target.at[2 * e + core], ss, rs, near_peer(kind, other)
                )

    def window(kind, buffer):
        return buffer.at[pl.ds(0, 2)] if kind == OWN_CHIP else buffer

    def dispatch(i):
        kind = chunks[i][0]
        out_slab, in_slab = bufs[i][:2]
        if not ready:
            pl.semaphore_wait(barrier, n_groups + n_width - 2)
            ready.append(True)
        exchange(kind, out_slab, in_slab, d_ss.at[i], d_rs.at[i])
        register(i)

    def register(i):
        kind = chunks[i][0]
        pending[("D", i)] = arrival(window(kind, bufs[i][0]), d_ss.at[i])
        sent[i] = [arrival(window(kind, bufs[i][1]), d_rs.at[i])]

    def from_ends(i):
        register(i)
        out_slab, in_slab = bufs[i][:2]

        def start():
            exchange(chunks[i][0], out_slab, in_slab, d_ss.at[i], d_rs.at[i])

        pl.when(pair == side)(start)

    def from_middle(i):
        out_slab, in_slab = bufs[i][:2]

        def start():
            exchange(chunks[i][0], out_slab, in_slab, d_ss.at[i], d_rs.at[i])

        pl.when(pair != side)(start)

    def mixers(i):
        mixed = jnp.concatenate(
            [jnp.where(hits(i, group), row_of(gate_of, i, group), 0.0) for group in range(half)],
            axis=0,
        )
        high = mixed.astype(bf16)
        mix = bufs[i][7]
        mix[0] = high
        mix[1] = (mixed - high.astype(f32)).astype(bf16)

    def settle(i):
        pending.pop(("D", i)).wait()

    loaded = set()

    def weight_ready(local_idx, which):
        if (local_idx, which) not in loaded:
            loaded.add((local_idx, which))
            weight_copies[local_idx * 3 + which].wait()

    part_sent, hid_sent, back_sent = {}, {}, {}
    combined = []
    tile = 256 if hidden_units % 256 == 0 else 128

    def gate_up(i):
        _, _, _, count = chunks[i]
        _, in_slab, part, _, _, _, _, _, sq, sq_in = bufs[i]
        for copy in sent[i]:
            copy.wait()
        values = in_slab[...].reshape(half * count, width_loc).astype(f32)
        rows = (values * gain_ref[...]).astype(bf16)
        for local_idx, groups in expert_groups(i):
            weight_ready(local_idx, 0)
            weight_ready(local_idx, 1)
            used = rows[groups.start * count : groups.stop * count]
            for which, weight in enumerate((wg, wu)):
                for begin in range(0, hidden_units, tile):
                    block = lax.dot_general(
                        used,
                        weight[local_idx, begin : begin + tile, :],
                        (((1,), (1,)), ((), ())),
                        preferred_element_type=f32,
                    ).astype(bf16)
                    column = which * hidden_units + begin
                    part[groups, :, column : column + tile] = block.reshape(-1, count, tile)
        squares = jnp.sum(values * values, axis=1, keepdims=True)
        owned = half * count // n_width
        for who in range(n_width):
            column = jnp.broadcast_to(squares[who * owned : (who + 1) * owned], (owned, 128))
            if owned < 128:
                column = jnp.concatenate([column, jnp.zeros((128 - owned, 128), f32)], axis=0)
            sq[who] = column.T[0:8]
        for step in (2, 1, 3)[: n_width - 1]:
            dest = lax.rem(tp + step, n_width)
            send(sq.at[dest], sq_in.at[step - 1], sq_ss.at[i], sq_rs.at[i], tp_peer(step))
            send(part.at[dest], bufs[i][3].at[step - 1], p_ss.at[i], p_rs.at[i], tp_peer(step))
        pending[("Q", i)] = arrival(sq_in, sq_ss.at[i])
        pending[("P", i)] = arrival(bufs[i][3], p_ss.at[i])
        part_sent[i] = [arrival(sq_in, sq_rs.at[i]), arrival(bufs[i][3], p_rs.at[i])]

    def hidden(i):
        _, _, part, part_in, hid, _, _, _, sq, sq_in = bufs[i]
        for copy in part_sent[i]:
            copy.wait()
        owned = part.shape[1]
        total = sq[tp]
        for step in range(1, n_width):
            total = total + sq_in[step - 1]
        total = jnp.broadcast_to(total[0:1], (128, 128)).T[0:owned, 0:1]
        inverse = lax.rsqrt(total / (width_loc * n_width) + EPSILON)
        for begin in range(0, hidden_units, tile):
            sums = []
            for column in (begin, hidden_units + begin):
                value = part[tp, :, column : column + tile].astype(f32)
                for step in range(1, n_width):
                    value = value + part_in[step - 1, :, column : column + tile].astype(f32)
                sums.append(value * inverse)
            gate, up = sums
            hid[tp, :, begin : begin + tile] = (gate / (1.0 + jnp.exp(-gate)) * up).astype(bf16)
        pending.pop(("Q", i)).wait()
        for step in (2, 1, 3)[: n_width - 1]:
            send(hid.at[tp], hid.at[tp], sq_ss.at[i], h_rs.at[i], tp_peer(step))
        pending[("H", i)] = arrival(hid.at[pl.ds(0, n_width - 1)], sq_ss.at[i])
        hid_sent[i] = [arrival(hid.at[pl.ds(0, n_width - 1)], h_rs.at[i])]

    def down(i):
        kind, _, _, count = chunks[i]
        _, _, _, _, hid, result, back, _, _, _ = bufs[i]
        for copy in hid_sent[i]:
            copy.wait()
        for local_idx, groups in expert_groups(i):
            weight_ready(local_idx, 2)
            rows = hid[groups].reshape(-1, hidden_units)
            for begin in range(0, width_loc, 256):
                block = jnp.dot(
                    rows, wd[local_idx, :, begin : begin + 256], preferred_element_type=f32
                )
                result[groups, :, begin : begin + 256] = block.astype(bf16).reshape(-1, count, 256)
        pending.pop(("D", i)).wait()
        exchange(kind, result, back, d_ss.at[i], r_rs.at[i])
        pending[("R", i)] = arrival(window(kind, result), d_ss.at[i])
        back_sent[i] = [arrival(window(kind, back), r_rs.at[i])]
        keep_own(kind, result, back)

    def combine(i):
        _, _, _, count = chunks[i]
        _, _, _, _, _, _, back, mix, _, _ = bufs[i]
        for copy in back_sent[i]:
            copy.wait()
        combined.append(i)
        rows = back[...].reshape(half * count, width_loc)
        value = sum(
            lax.dot_general(mix[half], rows, (((0,), (0,)), ((), ())), preferred_element_type=f32)
            for half in range(2)
        )
        if len(combined) > 1:
            value = acc[...] + value
        if len(combined) < n_chunks:
            acc[...] = value
        else:
            out_ref[...] = value.astype(bf16)

    steps = {
        "D": pick, "X": dispatch, "E": from_ends, "N": from_middle, "M": mixers, "S": settle,
         "G": gate_up, "H": hidden, "W": down, "C": combine
    }
    input_copies[3].wait()
    for word in ORDER:
        steps[word[0]](int(word[1:]))
    for copy in pending.values():
        copy.wait()


ORDER = (
    "D0", "X0", "D4", "X4", "D5", "X5", "D1", "X1", "D2", "E2", "D3", "E3",
    "M0", "M1", "M2", "M3", "M4", "M5", "G4", "G0", "N2", "H4", "G5", "N3",
    "H0", "G1", "W4", "W0", "H1", "H5", "G2", "W1", "W5", "H2", "G3", "W2",
    "H3", "W3", "C4", "C5", "C0", "C1", "C2", "C3",
)


def kernel_shards(
    cuts, tokens, norm_gain, route_ids, route_gates, w_gate, w_up, w_down
):
    tok_rows, width_loc = tokens.shape
    exp_local, hidden_units, _ = w_gate.shape
    n_groups, n_width = lax.axis_size("ep"), lax.axis_size("tp")
    chunks = slot_chunks(cuts)
    half = n_groups // 2
    f32, bf16 = jnp.float32, jnp.bfloat16
    per_chunk = []
    for _, _, _, count in chunks:
        rows = half * count
        per_chunk += [
            pltpu.VMEM((half, count, width_loc), bf16),
            pltpu.VMEM((half, count, width_loc), bf16),
            pltpu.VMEM((n_width, rows // n_width, 2 * hidden_units), bf16),
            pltpu.VMEM((n_width - 1, rows // n_width, 2 * hidden_units), bf16),
            pltpu.VMEM((n_width, rows // n_width, hidden_units), bf16),
            pltpu.VMEM((half, count, width_loc), bf16),
            pltpu.VMEM((half, count, width_loc), bf16),
            pltpu.VMEM((2, rows, tok_rows), bf16),
            pltpu.VMEM((n_width, 8, 128), f32),
            pltpu.VMEM((n_width - 1, 8, 128), f32),
        ]
    operands = (
        tokens, norm_gain.reshape(1, width_loc), route_ids.T, route_gates.T, w_gate, w_up, w_down
    )
    n_chunks = len(chunks)
    sems = [pltpu.SemaphoreType.DMA((4,)), pltpu.SemaphoreType.DMA((exp_local, 3))]
    sems += [pltpu.SemaphoreType.DMA((n_chunks,))] * 8
    anywhere = pl.BlockSpec(memory_space=pl.ANY)
    return pl.pallas_call(
        functools.partial(experts_kernel, (n_groups, n_width, exp_local, chunks)),
        out_shape=jax.ShapeDtypeStruct((tok_rows, width_loc), bf16),
        in_specs=[anywhere] * 7,
        out_specs=pl.BlockSpec(memory_space=pltpu.VMEM),
        scratch_shapes=[
            pltpu.VMEM(tokens.shape, bf16),
            pltpu.VMEM((1, width_loc), f32),
            pltpu.VMEM(route_ids.shape[::-1], jnp.int32),
            pltpu.VMEM(route_gates.shape[::-1], f32),
            pltpu.VMEM(w_gate.shape, bf16),
            pltpu.VMEM(w_up.shape, bf16),
            pltpu.VMEM(w_down.shape, bf16),
            pltpu.VMEM((tok_rows, width_loc), f32),
            *per_chunk,
            *sems,
        ],
        compiler_params=pltpu.CompilerParams(
            collective_id=0, has_side_effects=True, vmem_limit_bytes=40 * 1024 * 1024
        ),
    )(*[pltpu.with_memory_space_constraint(array, pltpu.HBM) for array in operands])


def plan(capacity):
    if capacity % 8 or capacity < 24:
        return None
    large = capacity // 16 * 8 + 8
    pieces = (large, capacity - large)
    return (
        (REMOTE, 0, pieces),
        (REMOTE, 1, pieces),
        (OWN_CHIP, 0, (capacity,)),
        (NEXT_CHIP, 0, (capacity,)),
    )


def solution(mesh):
    placed = (
        P("ep", "tp"),
        P("tp"),
        P("ep", None),
        P("ep", None),
        P("ep", None, "tp"),
        P("ep", None, "tp"),
        P("ep", None, "tp"),
    )
    n_groups, n_width = mesh.shape["ep"], mesh.shape["tp"]

    def body(tokens, norm_gain, route_ids, route_gates, w_gate, w_up, w_down):
        experts = w_gate.shape[0] * n_groups
        tok_rows, width_loc = tokens.shape
        top_count = route_ids.shape[1]
        capacity = max(2, (5 * tok_rows * top_count + 4 * experts - 1) // (4 * experts))
        cuts = plan(capacity)
        arrays = (tokens, norm_gain, route_ids, route_gates, w_gate, w_up, w_down)
        fits = n_groups == 8 and n_width == 4 and w_gate.shape[0] == 2 and capacity <= 128
        if cuts is None or not fits or width_loc % 256 or tok_rows % 128:
            return shards(*arrays)
        return kernel_shards(cuts, *arrays)

    return jax.shard_map(
        body, mesh=mesh, in_specs=placed, out_specs=P("ep", "tp"), check_vma=False
    )
```
